32 devices in a mesh: sp: 16 (over z, y, x), tp: 2 (over core).
Axes of the slice: x: 2, y: 2, z: 4, core: 2. Of those that a mesh axis runs over, the one named last changes fastest.
Arguments:
- queries: bfloat16 [8192, 8, 128], P('sp', 'tp'), may hold values from -60 to 60
- keys: bfloat16 [8192, 8, 128], P('sp', 'tp'), may hold values from -40 to 40
- values: bfloat16 [8192, 8, 128], P('sp', 'tp'), may hold values from -6 to 6
- w_out: bfloat16 [1024, 2048], P(None, 'tp'), may hold values from -0.1875 to 0.1875
Outputs:
- mixed: bfloat16 [8192, 2048], P('sp', 'tp')
The draws below stay inside these ranges and needn't reach their ends.
All inputs are finite; a program needn't handle non-finite values.
Results may differ from the reference program's by a relative error of at most 0.0051.
Values may be sent and summed in bfloat16 or wider, within the bound.
A program may use at most 64 MiB of HBM per device.

```python
import math
import jax
import jax.numpy as jnp
from jax import lax

D = 2048
HEADS = 8
HEAD_DIM = 128
W1 = 128
WINDOW_TWO = 512
DILATION_TWO = 4
WINDOW_THREE = 2048
DILATION_THREE = 16
TOKENS = 8192


def drawn_pair(key):
    shape = (TOKENS, HEADS, HEAD_DIM)
    starting_keys = jax.random.normal(jax.random.fold_in(key, 11), shape, jnp.float32)
    base_queries = jax.random.normal(jax.random.fold_in(key, 12), shape, jnp.float32) * 2.5
    return (jnp.clip(base_queries, -60.0, 60.0), jnp.clip(starting_keys, -40.0, 40.0))


def draw_queries(key, part):
    return drawn_pair(key)[0].astype(jnp.bfloat16)


def draw_keys(key, part):
    return drawn_pair(key)[1].astype(jnp.bfloat16)


def shard_levels(stream_key, dims, split, low, largest):
    def one(position, parts):
        draws = jax.random.uniform(jax.random.fold_in(jax.random.fold_in(stream_key, 6), position), (parts,), jnp.float32, low / len(split), largest / len(split))
        return jnp.repeat(jnp.exp(draws), dims[position] // parts).reshape((-1,) + (1,) * (len(dims) - position - 1))

    gain = one(*split[0])
    for cut in split[1:]:
        gain = gain * one(*cut)
    return gain


def gaussian(stream_key, extent, deviation, bound, shards=(), kind=jnp.bfloat16):
    values = deviation * jax.random.normal(stream_key, extent, jnp.float32)
    if shards:
        values = values * shard_levels(stream_key, extent, shards, -0.22, 0.18)
    return jnp.clip(values, -bound, bound).astype(kind)


def setup_inputs(seed: int = 0) -> dict:
    key_of = jax.random.split(jax.random.key(seed), 5)
    queries = draw_queries(jax.random.fold_in(key_of[4], 71), 0)
    keys = draw_keys(jax.random.fold_in(key_of[4], 71), 0)
    values = gaussian(key_of[2], (TOKENS, HEADS, HEAD_DIM), 1.0, 6.0, ((0, 16), (1, 2)))
    w_out = gaussian(key_of[3], (HEADS * HEAD_DIM, D), (HEADS * HEAD_DIM) ** -0.5, 0.1875, ((1, 2),))
    return dict(queries=queries, keys=keys, values=values, w_out=w_out)


def with_previous(blocks):
    earlier = jnp.concatenate([jnp.zeros_like(blocks[:1]), blocks[:-1]], axis=0)
    return jnp.concatenate([earlier, blocks], axis=1)

def single_branch(head_queries, head_keys, head_values, window, dilation):
    band_rows = window // dilation
    block_count = TOKENS // window
    shape = (block_count, band_rows, dilation, HEAD_DIM)
    query_blocks = head_queries.astype(jnp.float32).reshape(shape)
    key_bands = with_previous(head_keys.astype(jnp.float32).reshape(shape))
    value_bands = with_previous(head_values.astype(jnp.float32).reshape(shape))
    scores = jnp.einsum('nqrd,nkrd->nrqk', query_blocks, key_bands) / math.sqrt(HEAD_DIM)
    query_idx = jnp.arange(band_rows, dtype=jnp.int32)[:, None]
    key_idx = jnp.arange(2 * band_rows, dtype=jnp.int32)[None, :]
    distance = query_idx - key_idx + band_rows
    key_rows = jnp.arange(block_count, dtype=jnp.int32)[:, None, None] * band_rows - band_rows + key_idx[None]
    allowed = (distance >= 0)[None] & (distance <= band_rows)[None] & (key_rows >= 0)
    scores = jnp.where(allowed[:, None], scores, -jnp.inf)
    row_max = lax.optimization_barrier(jnp.max(scores, axis=-1, keepdims=True))
    numerators = jnp.exp(scores - row_max)
    row_sum = lax.optimization_barrier(jnp.sum(numerators, axis=-1, keepdims=True))
    rounded = lax.optimization_barrier(numerators.astype(jnp.bfloat16)).astype(jnp.float32)
    branch_out = jnp.einsum('nrqk,nkrd->nqrd', rounded, value_bands) / jnp.transpose(row_sum, (0, 2, 1, 3))
    log_total = jnp.transpose((row_max + jnp.log(row_sum))[..., 0], (0, 2, 1))
    return (branch_out.reshape(TOKENS, HEAD_DIM), log_total.reshape(TOKENS))

def one_head(operands):
    head_queries, head_keys, head_values = operands
    first_out, first_total = single_branch(head_queries, head_keys, head_values, W1, 1)
    second_output, second_branch_total = single_branch(head_queries, head_keys, head_values, WINDOW_TWO, DILATION_TWO)
    third_output, third_branch_total = single_branch(head_queries, head_keys, head_values, WINDOW_THREE, DILATION_THREE)
    weights = jax.nn.softmax(jnp.stack([first_total, second_branch_total, third_branch_total]), axis=0)
    stacked = jnp.stack([first_out, second_output, third_output])
    return lax.optimization_barrier(jnp.sum(weights[:, :, None] * stacked, axis=0))

def reference(queries, keys, values, w_out):
    per_head = lax.map(one_head, (jnp.transpose(queries, (1, 0, 2)), jnp.transpose(keys, (1, 0, 2)), jnp.transpose(values, (1, 0, 2))))
    attended = jnp.transpose(per_head, (1, 0, 2)).reshape(TOKENS, HEADS * HEAD_DIM).astype(jnp.bfloat16)
    return jnp.dot(attended, w_out, preferred_element_type=jnp.float32).astype(jnp.bfloat16)
```

```python
import functools
import math

import jax
import jax.numpy as jnp
from jax import lax
from jax.experimental import pallas as pl
from jax.experimental.pallas import tpu as pltpu
from jax.sharding import PartitionSpec as P

W1 = 128
WINDOW_TWO = 512
DILATION_TWO = 4
WINDOW_THREE = 2048
DILATION_THREE = 16
MESH = pl.DeviceIdType.MESH
RATIO = DILATION_THREE // DILATION_TWO
CHUNKS = DILATION_TWO
ROWS_ONE = 16
PARTS = 4
ROWS_TWO = WINDOW_TWO // DILATION_THREE


def attend(blocks, scale):
    scores = [
        lax.dot_general(q, k, (((1,), (1,)), ((), ())), preferred_element_type=jnp.float32)
        for q, k, _, _ in blocks
    ]
    scores = [x * scale + bias for x, (_, _, _, bias) in zip(scores, blocks)]
    tops = [jnp.max(x, axis=-1, keepdims=True) for x in scores]
    numerators = [jnp.exp2(x - top) for x, top in zip(scores, tops)]
    sums = [
        jnp.dot(
            x.astype(v.dtype), jnp.concatenate([v, jnp.ones_like(v)], axis=1), preferred_element_type=jnp.float32
        )
        for x, (_, _, v, _) in zip(numerators, blocks)
    ]
    dim = blocks[0][2].shape[-1]
    return [(x[:, :dim], jnp.broadcast_to(top, x[:, :dim].shape), x[:, dim:]) for x, top in zip(sums, tops)]


def bias_of(shape, place_q, place_k, first_own, window, has_prev):
    query_place, _ = place_q(lax.broadcasted_iota(jnp.int32, shape, 0))
    key_place, key_row = place_k(lax.broadcasted_iota(jnp.int32, shape, 1))
    distance = query_place - key_place
    allowed = (distance >= 0) & (distance <= window)
    general = jnp.where(allowed, 0.0, -jnp.inf).astype(jnp.float32)
    gate = jnp.where(has_prev, 0, first_own)
    first = jnp.where(allowed & (key_row >= gate), 0.0, -jnp.inf).astype(jnp.float32)
    return general, first


def kernel(
    group, q_hbm, k_hbm, v_hbm, w_hbm, *refs
):
    o_refs = refs[:PARTS]
    (
    nat, raw, wide, q_ref, k_ref, v_ref, w_ref, qb, kb, vb, acc, mx, sm, ob, ab, bias1, bias1f, bias2, bias2f, bias3,
    load, in_send, in_recv, z_send, z_recv, zl_send, zl_recv, o_send, o_recv, d_send, d_recv,
    ) = refs[PARTS:]
    res, dim = DILATION_THREE, q_ref.shape[-1]
    piece = q_ref.shape[2]
    rows = group * piece
    sp, tp = lax.axis_index("sp"), lax.axis_index("tp")
    n_sp, n_tp = lax.axis_size("sp"), lax.axis_size("tp")
    mine = lax.rem(sp, group)
    base = sp - mine
    has_prev = sp >= group
    has_next = sp + group < n_sp
    partner = n_tp - 1 - tp
    scale = math.log2(math.e) / math.sqrt(dim)

    loads = [
        pltpu.make_async_copy(source, place, load.at[i])
        for i, (source, place) in enumerate(
            ((k_hbm, raw.at[0]), (v_hbm, raw.at[1]), (q_hbm, raw.at[2]), (w_hbm, w_ref))
        )
    ]
    barrier = pltpu.get_barrier_semaphore()
    for d in range(1, group):
        pl.semaphore_signal(
            barrier, inc=1, device_id={"sp": base + lax.rem(mine + d, group)}, device_id_type=MESH
        )
    pl.semaphore_signal(barrier, inc=1, device_id={"tp": partner}, device_id_type=MESH)

    @pl.when(has_prev)
    def _():
        pl.semaphore_signal(barrier, inc=1, device_id={"sp": sp - group}, device_id_type=MESH)

    @pl.when(has_next)
    def _():
        pl.semaphore_signal(barrier, inc=1, device_id={"sp": sp + group}, device_id_type=MESH)

    for copy in loads:
        copy.start()

    def span(start):
        return pl.ds(pl.multiple_of(start, piece), piece)

    tensors = ((k_ref, kb, rows), (v_ref, vb, rows), (q_ref, qb, 0))

    def member(d):
        other, bit = mine, 1
        while bit <= d:
            if d & bit:
                other = other + bit * (1 - 2 * lax.rem(mine // bit, 2))
            bit *= 2
        return other

    def exchange(which, d):
        source, buffer, offset = tensors[which]
        other = member(d)
        return pltpu.make_async_remote_copy(
            src_ref=source.at[other],
            dst_ref=buffer.at[:, span(offset + piece * mine), :],
            send_sem=in_send.at[which, d],
            recv_sem=in_recv.at[which, d],
            device_id={"sp": base + other},
            device_id_type=MESH,
        )

    def arrival(which, d):
        source, buffer, offset = tensors[which]
        return pltpu.make_async_remote_copy(
            src_ref=source.at[0],
            dst_ref=buffer.at[:, span(offset + piece * member(d)), :],
            send_sem=in_send.at[which, d],
            recv_sem=in_recv.at[which, d],
            device_id={"sp": sp},
            device_id_type=MESH,
        )

    low = piece - ROWS_ONE

    def onward_rows(which, k):
        source, buffer, _ = tensors[which]
        start = piece * member(k)
        if k == 0:
            src, dst = source.at[mine], buffer.at[:, span(start), :]
        elif k in whole:
            src, dst = buffer.at[:, span(rows + start), :], buffer.at[:, span(start), :]
        else:
            ends = [pl.ds(pl.multiple_of(x + start + low, ROWS_ONE), ROWS_ONE) for x in (rows, 0)]
            src, dst = (buffer.at[:, x, :] for x in ends)
        return pltpu.make_async_remote_copy(
            src_ref=src,
            dst_ref=dst,
            send_sem=z_send.at[which, k],
            recv_sem=z_recv.at[which, k],
            device_id={"sp": sp + group},
            device_id_type=MESH,
        )

    def onward_chunk(which, k, s):
        _, buffer, _ = tensors[which]
        start = piece * member(k)
        part = pl.ds(s * RATIO, RATIO)
        return pltpu.make_async_remote_copy(
            src_ref=buffer.at[part, pl.ds(pl.multiple_of(rows + start, ROWS_ONE), low), :],
            dst_ref=buffer.at[part, pl.ds(pl.multiple_of(start, ROWS_ONE), low), :],
            send_sem=zl_send.at[which, k, s],
            recv_sem=zl_recv.at[which, k, s],
            device_id={"sp": sp + group},
            device_id_type=MESH,
        )

    whole = range(group // 2)
    split = range(group // 2, group)

    near = [d for d in range(1, group) if d & (d - 1) == 0]
    far = [d for d in range(1, group) if d & (d - 1)]
    pad = (res + 1) * group
    for which, (source, buffer, offset) in enumerate(tensors):
        loads[which].wait()
        for i in range(piece):
            tokens = raw[which, pl.ds(i * res, res)].astype(jnp.float32)
            wide[which, pl.ds(i * pad, res * group), :] = tokens.reshape(res * group, dim)
        for h in range(group):
            for r in range(res):
                store = r % DILATION_TWO * RATIO + r // DILATION_TWO
                rows_of = wide[which, pl.ds(r * group + h, piece, stride=pad), :]
                source[h, store] = rows_of.astype(source.dtype)
        buffer[:, span(offset + piece * mine), :] = source[mine]

    @pl.when(jnp.logical_not(has_prev))
    def _():
        kb[:, :rows, :] = jnp.zeros((res, rows, dim), kb.dtype)
        vb[:, :rows, :] = jnp.zeros((res, rows, dim), vb.dtype)

    def place_one(per):
        def place(i):
            store, row = i // per, i % per
            residue = (store % RATIO) * DILATION_TWO + store // RATIO
            return row * res + residue, row
        return place

    def place_two(per):
        def place(i):
            j, row = i // per, i % per
            return row * RATIO + j, row
        return place

    def shifted(place, by):
        def moved(i):
            at, row = place(i)
            return at + by, row
        return moved

    bias1[...], bias1f[...] = bias_of(
        bias1.shape, shifted(place_one(ROWS_ONE), ROWS_ONE * res), place_one(2 * ROWS_ONE), ROWS_ONE, W1, has_prev
    )
    bias2[...], bias2f[...] = bias_of(
        bias2.shape, shifted(place_two(ROWS_TWO), ROWS_TWO * RATIO), place_two(2 * ROWS_TWO), ROWS_TWO,
        WINDOW_TWO // DILATION_TWO, has_prev,
    )
    _, bias3[...] = bias_of(
        bias3.shape, lambda i: (i + rows, i), lambda i: (i, i), rows, WINDOW_THREE // DILATION_THREE, has_prev
    )

    pl.semaphore_wait(barrier, group + jnp.where(has_prev, 1, 0) + jnp.where(has_next, 1, 0))

    @pl.when(has_next)
    def _():
        for which in (0, 1):
            onward_rows(which, 0).start()

    for tensors_now in ((0, 1), (2,)):
        for members in (near, far):
            for which in tensors_now:
                for d in members:
                    exchange(which, d).start()

    for members in (near, far):
        for which in (0, 1):
            for k in members:
                arrival(which, k).wait_recv()

            @pl.when(has_next)
            def _():
                for k in members:
                    onward_rows(which, k).start()

    @pl.when(has_next)
    def _():
        for s in range(CHUNKS):
            for k in split:
                for which in (0, 1):
                    onward_chunk(which, k, s).start()

    def branch_one(blocks, bias):
        spans = [
            (
                pl.ds(pl.multiple_of(b * ROWS_ONE, ROWS_ONE), ROWS_ONE),
                pl.ds(pl.multiple_of(rows + (b - 1) * ROWS_ONE, ROWS_ONE), 2 * ROWS_ONE),
            )
            for b in blocks
        ]
        found = attend(
            [
                tuple(x[:, at, :].reshape(-1, dim) for x, at in ((qb, own), (kb, near), (vb, near))) + (bias[...],)
                for own, near in spans
            ],
            scale,
        )
        for (own, _), (weighted, top, total) in zip(spans, found):
            acc[:, own, :] = weighted.reshape(res, ROWS_ONE, dim)
            mx[:, own, :] = top.reshape(res, ROWS_ONE, dim)
            sm[:, own, :] = total.reshape(res, ROWS_ONE, dim)

    def merge(at, weighted, top, total):
        old_top = mx[at].reshape(-1, dim)
        new_top = jnp.maximum(old_top, top)
        old_part, part = jnp.exp2(old_top - new_top), jnp.exp2(top - new_top)
        return (
            acc[at].reshape(-1, dim) * old_part + weighted * part,
            new_top,
            sm[at].reshape(-1, dim) * old_part + total * part,
        )

    def branch_two(blocks, bias):
        spans = [
            (
                pl.ds(s * RATIO, RATIO),
                pl.ds(b * ROWS_TWO, ROWS_TWO),
                pl.ds(rows + (b - 1) * ROWS_TWO, 2 * ROWS_TWO),
            )
            for s, b in blocks
        ]
        found = attend(
            [
                tuple(x[part, at, :].reshape(-1, dim) for x, at in ((qb, own), (kb, near), (vb, near))) + (bias[...],)
                for part, own, near in spans
            ],
            scale,
        )
        merged = [merge((part, own, slice(None)), *one) for (part, own, _), one in zip(spans, found)]
        for (part, own, _), (weighted, top, total) in zip(spans, merged):
            acc[part, own, :] = weighted.reshape(RATIO, ROWS_TWO, dim)
            mx[part, own, :] = top.reshape(RATIO, ROWS_TWO, dim)
            sm[part, own, :] = total.reshape(RATIO, ROWS_TWO, dim)

    def some(items, count):
        return [items[i : i + count] for i in range(0, len(items), count)]

    steps = piece // ROWS_ONE
    for d in [0] + near + far:
        if d:
            arrival(2, d).wait_recv()
        for inner in range(1, steps):
            branch_one([member(d) * steps + inner], bias1)
    for b in range(steps, rows // ROWS_ONE, steps):
        branch_one([b], bias1)
    for blocks in some([(s, b) for s in range(CHUNKS) for b in range(1, rows // ROWS_TWO)], 2):
        branch_two(blocks, bias2)

    @pl.when(has_prev)
    def _():
        for k in range(group):
            for which in (0, 1):
                onward_rows(which, k).wait_recv()

    branch_one([0], bias1f)

    head = tp * group + mine

    def lanes(index):
        return pl.ds(pl.multiple_of(index * dim, dim), dim)

    def give(s, d):
        part = pl.ds(s * RATIO, RATIO)
        other = member(d)
        return pltpu.make_async_remote_copy(
            src_ref=ob.at[part, span(piece * other), :],
            dst_ref=ab.at[part, :, lanes(head)],
            send_sem=o_send.at[s, d],
            recv_sem=o_recv.at[s, d],
            device_id={"sp": base + other},
            device_id_type=MESH,
        )

    def taken(s, d):
        part = pl.ds(s * RATIO, RATIO)
        return pltpu.make_async_remote_copy(
            src_ref=ob.at[part, span(0), :],
            dst_ref=ab.at[part, :, lanes(tp * group + member(d))],
            send_sem=o_send.at[s, d],
            recv_sem=o_recv.at[s, d],
            device_id={"sp": sp},
            device_id_type=MESH,
        )

    def swap(s, d):
        part = pl.ds(s * RATIO, RATIO)
        slot = ab.at[part, :, lanes(tp * group + member(d))]
        return pltpu.make_async_remote_copy(
            src_ref=ob.at[part, span(piece * mine), :] if d == 0 else slot,
            dst_ref=slot,
            send_sem=d_send.at[s, d],
            recv_sem=d_recv.at[s, d],
            device_id={"tp": partner},
            device_id_type=MESH,
        )

    def swapped(s, d):
        part = pl.ds(s * RATIO, RATIO)
        return pltpu.make_async_remote_copy(
            src_ref=ob.at[part, span(0), :],
            dst_ref=ab.at[part, :, lanes(partner * group + member(d))],
            send_sem=d_send.at[s, d],
            recv_sem=d_recv.at[s, d],
            device_id={"tp": partner},
            device_id_type=MESH,
        )

    def hand_over(s):
        for d in range(1, group):
            taken(s, d).wait_recv()
            swap(s, d).start()

    def project(s):
        part = pl.ds(s * RATIO, RATIO)
        for d in range(group):
            swapped(s, d).wait_recv()
        attended = ab[part].reshape(RATIO * piece, -1)
        mixed = jnp.dot(attended, w_ref[...], preferred_element_type=jnp.float32)
        for c in range(mixed.shape[1] // dim):
            for j in range(RATIO):
                at = pl.ds(s + DILATION_TWO * j, piece, stride=res + 1)
                nat[c, at, :] = mixed[j * piece : (j + 1) * piece, c * dim : (c + 1) * dim]

    for s in range(CHUNKS):
        part = pl.ds(s * RATIO, RATIO)

        @pl.when(has_prev)
        def _():
            for k in split:
                for which in (0, 1):
                    onward_chunk(which, k, s).wait_recv()

        branch_two([(s, 0)], bias2f)
        for stores in some(list(range(s * RATIO, (s + 1) * RATIO)), 2):
            found = attend([(qb[x], kb[x], vb[x], bias3[...]) for x in stores], scale)
            for x, one in zip(stores, found):
                weighted, _, total = merge((x,), *one)
                ob[x] = (weighted / total).astype(ob.dtype)
        for d in far + near:
            give(s, d).start()
        swap(s, 0).start()
        ab[part, :, lanes(head)] = ob[part, span(piece * mine), :]
        if s >= 2:
            hand_over(s - 2)
    loads[3].wait()
    for s in range(CHUNKS - 2, CHUNKS):
        hand_over(s)
        project(s - 2)
    for s in range(CHUNKS - 2, CHUNKS):
        project(s)

    per = piece // PARTS
    for i in range(piece):
        for c in range(nat.shape[0]):
            o_refs[i // per][i % per * res : i % per * res + res, c * dim : (c + 1) * dim] = nat[
                c, i * (res + 1) : i * (res + 1) + res, :
            ].astype(jnp.bfloat16)

    for which in (0, 1, 2):
        for d in range(1, group):
            exchange(which, d).wait_send()

    @pl.when(has_next)
    def _():
        for which in (0, 1):
            for k in range(group):
                onward_rows(which, k).wait_send()
            for k in split:
                for s in range(CHUNKS):
                    onward_chunk(which, k, s).wait_send()

    for s in range(CHUNKS):
        for d in range(1, group):
            give(s, d).wait_send()
        for d in range(group):
            swap(s, d).wait_send()


def local(queries, keys, values, w_out):
    tokens, group, dim = queries.shape
    features, columns = w_out.shape
    res = DILATION_THREE
    piece = tokens // res
    rows = group * piece
    assert group & (group - 1) == 0 and piece > ROWS_ONE
    assert group * tokens == WINDOW_THREE and lax.axis_size("sp") % group == 0 and lax.axis_size("tp") == 2

    low, full = jnp.bfloat16, jnp.float32
    dma = pltpu.SemaphoreType.DMA
    vmem = pl.BlockSpec(memory_space=pltpu.VMEM)
    hbm = pl.BlockSpec(memory_space=pltpu.HBM)
    mixed = pl.pallas_call(
        functools.partial(kernel, group),
        out_shape=[jax.ShapeDtypeStruct((tokens // PARTS, columns), low)] * PARTS,
        in_specs=[hbm] * 4,
        out_specs=[vmem] * PARTS,
        scratch_shapes=[
            pltpu.VMEM((columns // dim, piece * (res + 1), dim), full),
            pltpu.VMEM((3, tokens, group, dim), low),
            pltpu.VMEM((3, piece * (res + 1) * group, dim), full),
            pltpu.VMEM((group, res, piece, dim), low),
            pltpu.VMEM((group, res, piece, dim), low),
            pltpu.VMEM((group, res, piece, dim), low),
            pltpu.VMEM((features, columns), low),
            pltpu.VMEM((res, rows, dim), low),
            pltpu.VMEM((res, 2 * rows, dim), low),
            pltpu.VMEM((res, 2 * rows, dim), low),
            pltpu.VMEM((res, rows, dim), full),
            pltpu.VMEM((res, rows, dim), full),
            pltpu.VMEM((res, rows, dim), full),
            pltpu.VMEM((res, rows, dim), low),
            pltpu.VMEM((res, piece, features), low),
            pltpu.VMEM((res * ROWS_ONE, 2 * res * ROWS_ONE), full),
            pltpu.VMEM((res * ROWS_ONE, 2 * res * ROWS_ONE), full),
            pltpu.VMEM((RATIO * ROWS_TWO, 2 * RATIO * ROWS_TWO), full),
            pltpu.VMEM((RATIO * ROWS_TWO, 2 * RATIO * ROWS_TWO), full),
            pltpu.VMEM((rows, 2 * rows), full),
            dma((4,)),
            dma((3, group)), dma((3, group)),
            dma((2, group)), dma((2, group)),
            dma((2, group, CHUNKS)), dma((2, group, CHUNKS)),
            dma((CHUNKS, group)), dma((CHUNKS, group)),
            dma((CHUNKS, group)), dma((CHUNKS, group)),
        ],
        compiler_params=pltpu.CompilerParams(
            collective_id=0, has_side_effects=True, vmem_limit_bytes=55_000_000
        ),
    )(queries, keys, values, w_out)
    return jnp.concatenate(mixed, axis=0)


def solution(mesh):
    in_specs = (P("sp", "tp", None), P("sp", "tp", None), P("sp", "tp", None), P(None, "tp"))
    out_specs = P("sp", "tp")
    return jax.shard_map(local, mesh=mesh, in_specs=in_specs, out_specs=out_specs, check_vma=False)
```

```python
import functools
import math

import jax
import jax.numpy as jnp
from jax import lax
from jax.experimental import pallas as pl
from jax.experimental.pallas import tpu as pltpu
from jax.sharding import PartitionSpec as P

W1 = 128
WINDOW_TWO = 512
DILATION_TWO = 4
WINDOW_THREE = 2048
DILATION_THREE = 16
MESH = pl.DeviceIdType.MESH
RATIO = DILATION_THREE // DILATION_TWO
CHUNKS = DILATION_TWO
ROWS_ONE = 16
PARTS = 4
UNITS = ((0, 4), (4, 4), (8, 4), (12, 2), (14, 2))
ROWS_TWO = WINDOW_TWO // DILATION_THREE


def attend(blocks, scale):
    scores = [
        lax.dot_general(q, k, (((1,), (1,)), ((), ())), preferred_element_type=jnp.float32)
        for q, k, _, _ in blocks
    ]
    scores = [x * scale + bias for x, (_, _, _, bias) in zip(scores, blocks)]
    tops = [jnp.max(x, axis=-1, keepdims=True) for x in scores]
    numerators = [jnp.exp2(x - top) for x, top in zip(scores, tops)]
    sums = [
        jnp.dot(
            x.astype(v.dtype), jnp.concatenate([v, jnp.ones_like(v)], axis=1), preferred_element_type=jnp.float32
        )
        for x, (_, _, v, _) in zip(numerators, blocks)
    ]
    dim = blocks[0][2].shape[-1]
    return [(x[:, :dim], jnp.broadcast_to(top, x[:, :dim].shape), x[:, dim:]) for x, top in zip(sums, tops)]


def bias_of(shape, place_q, place_k, first_own, window, has_prev):
    query_place, _ = place_q(lax.broadcasted_iota(jnp.int32, shape, 0))
    key_place, key_row = place_k(lax.broadcasted_iota(jnp.int32, shape, 1))
    distance = query_place - key_place
    allowed = (distance >= 0) & (distance <= window)
    general = jnp.where(allowed, 0.0, -jnp.inf).astype(jnp.float32)
    gate = jnp.where(has_prev, 0, first_own)
    first = jnp.where(allowed & (key_row >= gate), 0.0, -jnp.inf).astype(jnp.float32)
    return general, first


def kernel(
    group, q_hbm, k_hbm, v_hbm, w_hbm, *refs
):
    o_refs = refs[:PARTS]
    (
    nat, raw, wide, q_ref, k_ref, v_ref, w_ref, qb, kb, vb, acc, mx, sm, ob, ab, bias1, bias2, bias2f, bias3,
    load, in_send, in_recv, q_send, q_recv, z_send, z_recv, zb_send, zb_recv, zc_send, zc_recv, o_send, o_recv, d_send, d_recv,
    ) = refs[PARTS:]
    res, dim = DILATION_THREE, q_ref.shape[-1]
    piece = q_ref.shape[2]
    rows = group * piece
    sp, tp = lax.axis_index("sp"), lax.axis_index("tp")
    n_sp, n_tp = lax.axis_size("sp"), lax.axis_size("tp")
    mine = lax.rem(sp, group)
    base = sp - mine
    has_prev = sp >= group
    has_next = sp + group < n_sp
    partner = n_tp - 1 - tp
    scale = math.log2(math.e) / math.sqrt(dim)

    loads = [
        pltpu.make_async_copy(source, place, load.at[i])
        for i, (source, place) in enumerate(
            ((k_hbm, raw.at[0]), (v_hbm, raw.at[1]), (q_hbm, raw.at[2]), (w_hbm, w_ref))
        )
    ]
    barrier = pltpu.get_barrier_semaphore()
    for d in range(1, group):
        pl.semaphore_signal(
            barrier, inc=1, device_id={"sp": base + lax.rem(mine + d, group)}, device_id_type=MESH
        )
    pl.semaphore_signal(barrier, inc=1, device_id={"tp": partner}, device_id_type=MESH)

    @pl.when(has_prev)
    def _():
        pl.semaphore_signal(barrier, inc=1, device_id={"sp": sp - group}, device_id_type=MESH)

    @pl.when(has_next)
    def _():
        pl.semaphore_signal(barrier, inc=1, device_id={"sp": sp + group}, device_id_type=MESH)

    for copy in loads:
        copy.start()

    def span(start):
        return pl.ds(pl.multiple_of(start, piece), piece)

    tensors = ((k_ref, kb, rows), (v_ref, vb, rows), (q_ref, qb, 0))

    def member(d):
        other, bit = mine, 1
        while bit <= d:
            if d & bit:
                other = other + bit * (1 - 2 * lax.rem(mine // bit, 2))
            bit *= 2
        return other

    def exchange(which, d, s=None):
        source, buffer, offset = tensors[which]
        other = member(d)
        part = slice(None) if s is None else pl.ds(s * RATIO, RATIO)
        return pltpu.make_async_remote_copy(
            src_ref=source.at[other, part],
            dst_ref=buffer.at[part, span(offset + piece * mine), :],
            send_sem=in_send.at[which, d] if s is None else q_send.at[s],
            recv_sem=in_recv.at[which, d] if s is None else q_recv.at[s],
            device_id={"sp": base + other},
            device_id_type=MESH,
        )

    def arrival(which, d, s=None):
        source, buffer, offset = tensors[which]
        part = slice(None) if s is None else pl.ds(s * RATIO, RATIO)
        return pltpu.make_async_remote_copy(
            src_ref=source.at[0, part],
            dst_ref=buffer.at[part, span(offset + piece * member(d)), :],
            send_sem=in_send.at[which, d] if s is None else q_send.at[s],
            recv_sem=in_recv.at[which, d] if s is None else q_recv.at[s],
            device_id={"sp": sp},
            device_id_type=MESH,
        )

    low = piece - ROWS_ONE

    last = group - 1
    swapped_roles = member(2) == last
    early = jnp.where(swapped_roles, member(2), member(3))
    late = jnp.where(swapped_roles, member(3), member(2))

    def onward(which, src, dst, send, recv):
        return pltpu.make_async_remote_copy(
            src_ref=src,
            dst_ref=dst,
            send_sem=send,
            recv_sem=recv,
            device_id={"sp": sp + group},
            device_id_type=MESH,
        )

    def onward_rows(which, k):
        source, buffer, _ = tensors[which]
        start = piece * (mine, member(1), early)[k]
        if k == 0:
            src, dst = source.at[mine], buffer.at[:, span(start), :]
        elif k == 1:
            src, dst = buffer.at[:, span(rows + start), :], buffer.at[:, span(start), :]
        else:
            ends = [pl.ds(pl.multiple_of(x + start + low, ROWS_ONE), ROWS_ONE) for x in (rows, 0)]
            src, dst = (buffer.at[:, x, :] for x in ends)
        return onward(which, src, dst, z_send.at[which, k], z_recv.at[which, k])

    def onward_early(which, u):
        _, buffer, _ = tensors[which]
        ends = [pl.ds(pl.multiple_of(x + piece * early, ROWS_ONE), low) for x in (rows, 0)]
        src, dst = (buffer.at[pl.ds(*UNITS[u]), x, :] for x in ends)
        return onward(which, src, dst, zc_send.at[which, u], zc_recv.at[which, u])

    def onward_late(which, u):
        _, buffer, _ = tensors[which]
        src, dst = (buffer.at[pl.ds(*UNITS[u]), span(x + piece * late), :] for x in (rows, 0))
        return onward(which, src, dst, zb_send.at[which, u], zb_recv.at[which, u])

    near = [d for d in range(1, group) if d & (d - 1) == 0]
    far = [d for d in range(1, group) if d & (d - 1)]
    pad = (res + 1) * group
    for which, (source, buffer, offset) in enumerate(tensors):
        loads[which].wait()
        for i in range(piece):
            tokens = raw[which, pl.ds(i * res, res)].astype(jnp.float32)
            wide[which, pl.ds(i * pad, res * group), :] = tokens.reshape(res * group, dim)
        for h in range(group):
            for r in range(res):
                store = r % DILATION_TWO * RATIO + r // DILATION_TWO
                rows_of = wide[which, pl.ds(r * group + h, piece, stride=pad), :]
                source[h, store] = rows_of.astype(source.dtype)
        buffer[:, span(offset + piece * mine), :] = source[mine]

    @pl.when(jnp.logical_not(has_prev))
    def _():
        kb[:, :rows, :] = jnp.zeros((res, rows, dim), kb.dtype)
        vb[:, :rows, :] = jnp.zeros((res, rows, dim), vb.dtype)

    def place_one(per):
        def place(i):
            store, row = i // per, i % per
            residue = (store % RATIO) * DILATION_TWO + store // RATIO
            return row * res + residue, row
        return place

    def place_two(per):
        def place(i):
            j, row = i // per, i % per
            return row * RATIO + j, row
        return place

    def shifted(place, by):
        def moved(i):
            at, row = place(i)
            return at + by, row
        return moved

    bias1[0], bias1[1] = bias_of(
        bias1.shape[1:], shifted(place_one(ROWS_ONE), ROWS_ONE * res), place_one(2 * ROWS_ONE), ROWS_ONE, W1, has_prev
    )
    bias2[...], bias2f[...] = bias_of(
        bias2.shape, shifted(place_two(ROWS_TWO), ROWS_TWO * RATIO), place_two(2 * ROWS_TWO), ROWS_TWO,
        WINDOW_TWO // DILATION_TWO, has_prev,
    )
    _, bias3[...] = bias_of(
        bias3.shape, lambda i: (i + rows, i), lambda i: (i, i), rows, WINDOW_THREE // DILATION_THREE, has_prev
    )

    pl.semaphore_wait(barrier, group + jnp.where(has_prev, 1, 0) + jnp.where(has_next, 1, 0))

    @pl.when(has_next)
    def _():
        for which in (0, 1):
            onward_rows(which, 0).start()

    for members in (near, far):
        for which in (0, 1):
            for d in members:
                exchange(which, d).start()

    def pass_on(*copies):
        @pl.when(has_next)
        def _():
            for copy in copies:
                copy.start()

    def one(b, first=0, s=None):
        own = pl.ds(pl.multiple_of(b * ROWS_ONE, ROWS_ONE), ROWS_ONE)
        near_rows = pl.ds(pl.multiple_of(rows + (b - 1) * ROWS_ONE, ROWS_ONE), 2 * ROWS_ONE)
        start, count = (0, res) if s is None else (s * RATIO, RATIO)
        part = pl.ds(start, count)

        def keep(found):
            for ref, value in zip((acc, mx, sm), found):
                ref[part, own, :] = value.reshape(count, ROWS_ONE, dim)

        block = (
            qb[part, own, :].reshape(-1, dim),
            kb[:, near_rows, :].reshape(-1, dim),
            vb[:, near_rows, :].reshape(-1, dim),
            bias1[first, pl.ds(start * ROWS_ONE, count * ROWS_ONE), :],
        )
        return block, keep

    def merge(at, weighted, top, total):
        old_top = mx[at].reshape(-1, dim)
        new_top = jnp.maximum(old_top, top)
        old_part, part = jnp.exp2(old_top - new_top), jnp.exp2(top - new_top)
        return (
            acc[at].reshape(-1, dim) * old_part + weighted * part,
            new_top,
            sm[at].reshape(-1, dim) * old_part + total * part,
        )

    def two(s, b, bias=None):
        bias = bias2 if bias is None else bias
        part = pl.ds(s * RATIO, RATIO)
        own = pl.ds(pl.multiple_of(b * ROWS_TWO, ROWS_TWO), ROWS_TWO)
        near_rows = pl.ds(pl.multiple_of(rows + (b - 1) * ROWS_TWO, ROWS_TWO), 2 * ROWS_TWO)

        def keep(found):
            merged = merge((part, own, slice(None)), *found)
            for ref, value in zip((acc, mx, sm), merged):
                ref[part, own, :] = value.reshape(RATIO, ROWS_TWO, dim)

        block = tuple(x[part, at, :].reshape(-1, dim) for x, at in ((qb, own), (kb, near_rows), (vb, near_rows)))
        return block + (bias[...],), keep

    def three(x):
        def keep(found):
            weighted, _, total = merge((x,), *found)
            ob[x] = (weighted / total).astype(ob.dtype)

        return (qb[x], kb[x], vb[x], bias3[...]), keep

    def run(*groups):
        parts = [item for items, _ in groups for item in items]
        found = iter(attend([block for block, _ in parts], scale))
        for items, after in groups:
            for _, keep in items:
                keep(next(found))
            after()

    def nothing():
        pass

    def some(items, count):
        return [items[i : i + count] for i in range(0, len(items), count)]

    steps = piece // ROWS_ONE
    soon = mine + 1 - mine % 2
    later = (group // 2, group - soon)
    near_far = 2 + jnp.where(mine == 1, 1, 0)
    edge = jnp.where(mine == last, 1, 0)
    for d in near:
        arrival(0, d).wait_recv()
    pass_on(onward_rows(0, 1))
    for d in near:
        arrival(1, d).wait_recv()
    pass_on(onward_rows(1, 1))
    for d in far:
        arrival(0, d).wait_recv()
    for d in near:
        exchange(2, d).start()
    for s in range(CHUNKS):
        for d in far:
            exchange(2, d, s).start()
    pass_on(onward_rows(0, 2), onward_late(0, 0), onward_early(0, 0))
    for d in far:
        arrival(1, d).wait_recv()
    pass_on(
        onward_rows(1, 2), onward_late(1, 0), onward_early(1, 0),
        *[f(x, u) for u in (1, 2) for f in (onward_late, onward_early) for x in (0, 1)],
        *[f(x, u) for f in (onward_early, onward_late) for u in (3, 4) for x in (0, 1)],
    )
    def inners(d, s=None):
        return [one(member(d) * steps + inner, 0, s) for inner in range(1, steps)]

    run((inners(0), nothing))
    for d in near:
        arrival(2, d).wait_recv()
    for d, b in zip(near, (soon, near_far)):
        run((inners(d) + [one(b * steps)], nothing))
    run(([two(s, soon) for s in range(CHUNKS)], nothing))

    @pl.when(has_prev)
    def _():
        for k in range(3):
            for which in (0, 1):
                onward_rows(which, k).wait_recv()

    def sooner(s):
        if s == CHUNKS:
            return []
        for d in far:
            arrival(2, d, s).wait_recv()
        found = []
        for d in far:
            found += inners(d, s) + [one(member(d) * steps, jnp.where(member(d) == 0, 1, 0), s)]
        return found + [two(s, b) for b in later]

    run(([one(edge * steps, 1 - edge)] + sooner(0), nothing))

    head = tp * group + mine

    def lanes(index):
        return pl.ds(pl.multiple_of(index * dim, dim), dim)

    def give(u, d):
        part = pl.ds(*UNITS[u])
        other = member(d)
        return pltpu.make_async_remote_copy(
            src_ref=ob.at[part, span(piece * other), :],
            dst_ref=ab.at[part, :, lanes(head)],
            send_sem=o_send.at[u, d],
            recv_sem=o_recv.at[u, d],
            device_id={"sp": base + other},
            device_id_type=MESH,
        )

    def taken(u, d):
        part = pl.ds(*UNITS[u])
        return pltpu.make_async_remote_copy(
            src_ref=ob.at[part, span(0), :],
            dst_ref=ab.at[part, :, lanes(tp * group + member(d))],
            send_sem=o_send.at[u, d],
            recv_sem=o_recv.at[u, d],
            device_id={"sp": sp},
            device_id_type=MESH,
        )

    def swap(u, d):
        part = pl.ds(*UNITS[u])
        slot = ab.at[part, :, lanes(tp * group + member(d))]
        return pltpu.make_async_remote_copy(
            src_ref=ob.at[part, span(piece * mine), :] if d == 0 else slot,
            dst_ref=slot,
            send_sem=d_send.at[u, d],
            recv_sem=d_recv.at[u, d],
            device_id={"tp": partner},
            device_id_type=MESH,
        )

    def swapped(u, d):
        part = pl.ds(*UNITS[u])
        return pltpu.make_async_remote_copy(
            src_ref=ob.at[part, span(0), :],
            dst_ref=ab.at[part, :, lanes(partner * group + member(d))],
            send_sem=d_send.at[u, d],
            recv_sem=d_recv.at[u, d],
            device_id={"tp": partner},
            device_id_type=MESH,
        )

    def hand_over(u):
        for d in range(1, group):
            taken(u, d).wait_recv()
            swap(u, d).start()

    def project(u):
        start, count = UNITS[u]
        for d in range(group):
            swapped(u, d).wait_recv()
        attended = ab[pl.ds(start, count)].reshape(count * piece, -1)
        mixed = jnp.dot(attended, w_ref[...], preferred_element_type=jnp.float32)
        for c in range(mixed.shape[1] // dim):
            for j in range(count):
                residue = (start + j) // RATIO + (start + j) % RATIO * DILATION_TWO
                at = pl.ds(residue, piece, stride=res + 1)
                nat[c, at, :] = mixed[j * piece : (j + 1) * piece, c * dim : (c + 1) * dim]

    def from_prev(*copies):
        @pl.when(has_prev)
        def _():
            for copy in copies:
                copy.wait_recv()

    def hand_out(u):
        def now():
            part = pl.ds(*UNITS[u])
            for d in far + near:
                give(u, d).start()
            swap(u, 0).start()
            ab[part, :, lanes(head)] = ob[part, span(piece * mine), :]

        return now

    def threes(u):
        start, count = UNITS[u]
        return [three(x) for x in range(start, start + count)]

    for s in range(CHUNKS):
        units = [u for u, (start, _) in enumerate(UNITS) if start // RATIO == s]
        from_prev(*[onward_early(x, u) for u in units for x in (0, 1)])
        from_prev(*[onward_late(x, units[0]) for x in (0, 1)])
        run(
            ([two(s, 0, bias2f)] + threes(units[0]), hand_out(units[0])),
            (sooner(s + 1), nothing),
        )
        for u in units[1:]:
            from_prev(*[onward_late(x, u) for x in (0, 1)])
            run((threes(u), hand_out(u)))
        if s == 2:
            hand_over(0)
    loads[3].wait()
    for u in range(1, len(UNITS)):
        hand_over(u)
        project(u - 1)
    project(len(UNITS) - 1)

    per = piece // PARTS
    for i in range(piece):
        for c in range(nat.shape[0]):
            o_refs[i // per][i % per * res : i % per * res + res, c * dim : (c + 1) * dim] = nat[
                c, i * (res + 1) : i * (res + 1) + res, :
            ].astype(jnp.bfloat16)

    for which in (0, 1):
        for d in range(1, group):
            exchange(which, d).wait_send()
    for d in near:
        exchange(2, d).wait_send()
    for d in far:
        for s in range(CHUNKS):
            exchange(2, d, s).wait_send()

    @pl.when(has_next)
    def _():
        for which in (0, 1):
            for k in range(3):
                onward_rows(which, k).wait_send()
            for u in range(len(UNITS)):
                onward_early(which, u).wait_send()
                onward_late(which, u).wait_send()

    for u in range(len(UNITS)):
        for d in range(1, group):
            give(u, d).wait_send()
        for d in range(group):
            swap(u, d).wait_send()


def local(queries, keys, values, w_out):
    tokens, group, dim = queries.shape
    features, columns = w_out.shape
    res = DILATION_THREE
    piece = tokens // res
    rows = group * piece
    assert group == 4 and piece > ROWS_ONE
    assert group * tokens == WINDOW_THREE and lax.axis_size("sp") % group == 0 and lax.axis_size("tp") == 2

    low, full = jnp.bfloat16, jnp.float32
    dma = pltpu.SemaphoreType.DMA
    vmem = pl.BlockSpec(memory_space=pltpu.VMEM)
    hbm = pl.BlockSpec(memory_space=pltpu.HBM)
    mixed = pl.pallas_call(
        functools.partial(kernel, group),
        out_shape=[jax.ShapeDtypeStruct((tokens // PARTS, columns), low)] * PARTS,
        in_specs=[hbm] * 4,
        out_specs=[vmem] * PARTS,
        scratch_shapes=[
            pltpu.VMEM((columns // dim, piece * (res + 1), dim), full),
            pltpu.VMEM((3, tokens, group, dim), low),
            pltpu.VMEM((3, piece * (res + 1) * group, dim), full),
            pltpu.VMEM((group, res, piece, dim), low),
            pltpu.VMEM((group, res, piece, dim), low),
            pltpu.VMEM((group, res, piece, dim), low),
            pltpu.VMEM((features, columns), low),
            pltpu.VMEM((res, rows, dim), low),
            pltpu.VMEM((res, 2 * rows, dim), low),
            pltpu.VMEM((res, 2 * rows, dim), low),
            pltpu.VMEM((res, rows, dim), full),
            pltpu.VMEM((res, rows, dim), full),
            pltpu.VMEM((res, rows, dim), full),
            pltpu.VMEM((res, rows, dim), low),
            pltpu.VMEM((res, piece, features), low),
            pltpu.VMEM((2, res * ROWS_ONE, 2 * res * ROWS_ONE), full),
            pltpu.VMEM((RATIO * ROWS_TWO, 2 * RATIO * ROWS_TWO), full),
            pltpu.VMEM((RATIO * ROWS_TWO, 2 * RATIO * ROWS_TWO), full),
            pltpu.VMEM((rows, 2 * rows), full),
            dma((4,)),
            dma((3, group)), dma((3, group)),
            dma((CHUNKS,)), dma((CHUNKS,)),
            dma((2, 3)), dma((2, 3)),
            dma((2, len(UNITS))), dma((2, len(UNITS))),
            dma((2, len(UNITS))), dma((2, len(UNITS))),
            dma((len(UNITS), group)), dma((len(UNITS), group)),
            dma((len(UNITS), group)), dma((len(UNITS), group)),
        ],
        compiler_params=pltpu.CompilerParams(
            collective_id=0, has_side_effects=True, vmem_limit_bytes=55_000_000
        ),
    )(queries, keys, values, w_out)
    return jnp.concatenate(mixed, axis=0)


def solution(mesh):
    in_specs = (P("sp", "tp", None), P("sp", "tp", None), P("sp", "tp", None), P(None, "tp"))
    out_specs = P("sp", "tp")
    return jax.shard_map(local, mesh=mesh, in_specs=in_specs, out_specs=out_specs, check_vma=False)
```

```python
import functools
import math

import jax
import jax.numpy as jnp
from jax import lax
from jax.experimental import pallas as pl
from jax.experimental.pallas import tpu as pltpu
from jax.sharding import PartitionSpec as P

W1 = 128
WINDOW_TWO = 512
DILATION_TWO = 4
WINDOW_THREE = 2048
DILATION_THREE = 16
MESH = pl.DeviceIdType.MESH
RATIO = DILATION_THREE // DILATION_TWO
CHUNKS = DILATION_TWO
ROWS_ONE = 16
PARTS = 2
QUERY_PARTS = ((0, 1), (1, 3))
UNITS = ((0, 4), (4, 4), (8, 4), (12, 2), (14, 2))
ROWS_TWO = WINDOW_TWO // DILATION_THREE


def attend(blocks, scale):
    scores = [
        lax.dot_general(q, k, (((1,), (1,)), ((), ())), preferred_element_type=jnp.float32)
        for q, k, _, _ in blocks
    ]
    scores = [x * scale + bias for x, (_, _, _, bias) in zip(scores, blocks)]
    tops = [jnp.max(x, axis=-1, keepdims=True) for x in scores]
    numerators = [jnp.exp2(x - top) for x, top in zip(scores, tops)]
    sums = [jnp.sum(x, axis=-1, keepdims=True) for x in numerators]
    weighted = [
        jnp.dot(x.astype(v.dtype), v, preferred_element_type=jnp.float32)
        for x, (_, _, v, _) in zip(numerators, blocks)
    ]
    return [
        (x, jnp.broadcast_to(top, x.shape), jnp.broadcast_to(total, x.shape))
        for x, top, total in zip(weighted, tops, sums)
    ]


def bias_of(shape, place_q, place_k, first_own, window, has_prev):
    query_place, _ = place_q(lax.broadcasted_iota(jnp.int32, shape, 0))
    key_place, key_row = place_k(lax.broadcasted_iota(jnp.int32, shape, 1))
    distance = query_place - key_place
    allowed = (distance >= 0) & (distance <= window)
    general = jnp.where(allowed, 0.0, -jnp.inf).astype(jnp.float32)
    gate = jnp.where(has_prev, 0, first_own)
    first = jnp.where(allowed & (key_row >= gate), 0.0, -jnp.inf).astype(jnp.float32)
    return general, first


def kernel(
    group, q_hbm, k_hbm, v_hbm, w_hbm, *refs
):
    o_refs = refs[:PARTS]
    (
    nat, raw, wide, q_ref, k_ref, v_ref, w_ref, qb, kb, vb, acc, mx, sm, ob, ab, bias1, bias2, bias2f, bias3,
    load, in_send, in_recv, q_send, q_recv, z_send, z_recv, zb_send, zb_recv, zc_send, zc_recv, o_send, o_recv, d_send, d_recv,
    ) = refs[PARTS:]
    res, dim = DILATION_THREE, q_ref.shape[-1]
    piece = q_ref.shape[2]
    rows = group * piece
    sp, tp = lax.axis_index("sp"), lax.axis_index("tp")
    n_sp, n_tp = lax.axis_size("sp"), lax.axis_size("tp")
    mine = lax.rem(sp, group)
    base = sp - mine
    has_prev = sp >= group
    has_next = sp + group < n_sp
    partner = n_tp - 1 - tp
    scale = math.log2(math.e) / math.sqrt(dim)

    loads = [
        pltpu.make_async_copy(source, place, load.at[i])
        for i, (source, place) in enumerate(
            ((k_hbm, raw.at[0]), (v_hbm, raw.at[1]), (q_hbm, raw.at[2]), (w_hbm, w_ref))
        )
    ]
    barrier = pltpu.get_barrier_semaphore()
    for d in range(1, group):
        pl.semaphore_signal(
            barrier, inc=1, device_id={"sp": base + lax.rem(mine + d, group)}, device_id_type=MESH
        )
    pl.semaphore_signal(barrier, inc=1, device_id={"tp": partner}, device_id_type=MESH)

    @pl.when(has_prev)
    def _():
        pl.semaphore_signal(barrier, inc=1, device_id={"sp": sp - group}, device_id_type=MESH)

    @pl.when(has_next)
    def _():
        pl.semaphore_signal(barrier, inc=1, device_id={"sp": sp + group}, device_id_type=MESH)

    for copy in loads:
        copy.start()

    def span(start):
        return pl.ds(pl.multiple_of(start, piece), piece)

    tensors = ((k_ref, kb, rows), (v_ref, vb, rows), (q_ref, qb, 0))

    def member(d):
        other, bit = mine, 1
        while bit <= d:
            if d & bit:
                other = other + bit * (1 - 2 * lax.rem(mine // bit, 2))
            bit *= 2
        return other

    def exchange(which, d, s=None):
        source, buffer, offset = tensors[which]
        other = member(d)
        part = slice(None) if s is None else pl.ds(*(x * RATIO for x in QUERY_PARTS[s]))
        return pltpu.make_async_remote_copy(
            src_ref=source.at[other, part],
            dst_ref=buffer.at[part, span(offset + piece * mine), :],
            send_sem=in_send.at[which, d] if s is None else q_send.at[s],
            recv_sem=in_recv.at[which, d] if s is None else q_recv.at[s],
            device_id={"sp": base + other},
            device_id_type=MESH,
        )

    def arrival(which, d, s=None):
        source, buffer, offset = tensors[which]
        part = slice(None) if s is None else pl.ds(*(x * RATIO for x in QUERY_PARTS[s]))
        return pltpu.make_async_remote_copy(
            src_ref=source.at[0, part],
            dst_ref=buffer.at[part, span(offset + piece * member(d)), :],
            send_sem=in_send.at[which, d] if s is None else q_send.at[s],
            recv_sem=in_recv.at[which, d] if s is None else q_recv.at[s],
            device_id={"sp": sp},
            device_id_type=MESH,
        )

    low = piece - ROWS_ONE

    last = group - 1
    swapped_roles = member(2) == last
    early = jnp.where(swapped_roles, member(2), member(3))
    late = jnp.where(swapped_roles, member(3), member(2))

    def onward(which, src, dst, send, recv):
        return pltpu.make_async_remote_copy(
            src_ref=src,
            dst_ref=dst,
            send_sem=send,
            recv_sem=recv,
            device_id={"sp": sp + group},
            device_id_type=MESH,
        )

    def onward_rows(which, k):
        source, buffer, _ = tensors[which]
        start = piece * (mine, member(1), early)[k]
        if k == 0:
            src, dst = source.at[mine], buffer.at[:, span(start), :]
        elif k == 1:
            src, dst = buffer.at[:, span(rows + start), :], buffer.at[:, span(start), :]
        else:
            ends = [pl.ds(pl.multiple_of(x + start + low, ROWS_ONE), ROWS_ONE) for x in (rows, 0)]
            src, dst = (buffer.at[:, x, :] for x in ends)
        return onward(which, src, dst, z_send.at[which, k], z_recv.at[which, k])

    def onward_early(which, u):
        _, buffer, _ = tensors[which]
        ends = [pl.ds(pl.multiple_of(x + piece * early, ROWS_ONE), low) for x in (rows, 0)]
        src, dst = (buffer.at[pl.ds(*UNITS[u]), x, :] for x in ends)
        return onward(which, src, dst, zc_send.at[which, u], zc_recv.at[which, u])

    def onward_late(which, u):
        _, buffer, _ = tensors[which]
        src, dst = (buffer.at[pl.ds(*UNITS[u]), span(x + piece * late), :] for x in (rows, 0))
        return onward(which, src, dst, zb_send.at[which, u], zb_recv.at[which, u])

    near = [d for d in range(1, group) if d & (d - 1) == 0]
    far = [d for d in range(1, group) if d & (d - 1)]
    pad = (res + 1) * group
    for which, (source, buffer, offset) in enumerate(tensors):
        loads[which].wait()
        for i in range(piece):
            tokens = raw[which, pl.ds(i * res, res)].astype(jnp.float32)
            wide[which, pl.ds(i * pad, res * group), :] = tokens.reshape(res * group, dim)
        for h in range(group):
            for r in range(res):
                store = r % DILATION_TWO * RATIO + r // DILATION_TWO
                rows_of = wide[which, pl.ds(r * group + h, piece, stride=pad), :]
                source[h, store] = rows_of.astype(source.dtype)
        buffer[:, span(offset + piece * mine), :] = source[mine]

    @pl.when(jnp.logical_not(has_prev))
    def _():
        kb[:, :rows, :] = jnp.zeros((res, rows, dim), kb.dtype)
        vb[:, :rows, :] = jnp.zeros((res, rows, dim), vb.dtype)

    def place_one(per):
        def place(i):
            store, row = i // per, i % per
            residue = (store % RATIO) * DILATION_TWO + store // RATIO
            return row * res + residue, row
        return place

    def place_two(per):
        def place(i):
            j, row = i // per, i % per
            return row * RATIO + j, row
        return place

    def shifted(place, by):
        def moved(i):
            at, row = place(i)
            return at + by, row
        return moved

    bias1[0], bias1[1] = bias_of(
        bias1.shape[1:], shifted(place_one(ROWS_ONE), ROWS_ONE * res), place_one(2 * ROWS_ONE), ROWS_ONE, W1, has_prev
    )
    bias2[...], bias2f[...] = bias_of(
        bias2.shape, shifted(place_two(ROWS_TWO), ROWS_TWO * RATIO), place_two(2 * ROWS_TWO), ROWS_TWO,
        WINDOW_TWO // DILATION_TWO, has_prev,
    )
    _, bias3[...] = bias_of(
        bias3.shape, lambda i: (i + rows, i), lambda i: (i, i), rows, WINDOW_THREE // DILATION_THREE, has_prev
    )

    pl.semaphore_wait(barrier, group + jnp.where(has_prev, 1, 0) + jnp.where(has_next, 1, 0))

    @pl.when(has_next)
    def _():
        for which in (0, 1):
            onward_rows(which, 0).start()

    for members in (near, far):
        for which in (0, 1):
            for d in members:
                exchange(which, d).start()

    def pass_on(*copies):
        @pl.when(has_next)
        def _():
            for copy in copies:
                copy.start()

    def one(b, first=0, s=None):
        own = pl.ds(pl.multiple_of(b * ROWS_ONE, ROWS_ONE), ROWS_ONE)
        near_rows = pl.ds(pl.multiple_of(rows + (b - 1) * ROWS_ONE, ROWS_ONE), 2 * ROWS_ONE)
        start, count = (0, res) if s is None else (x * RATIO for x in QUERY_PARTS[s])
        part = pl.ds(start, count)

        def keep(found):
            for ref, value in zip((acc, mx, sm), found):
                ref[part, own, :] = value.reshape(count, ROWS_ONE, dim)

        block = (
            qb[part, own, :].reshape(-1, dim),
            kb[:, near_rows, :].reshape(-1, dim),
            vb[:, near_rows, :].reshape(-1, dim),
            bias1[first, pl.ds(start * ROWS_ONE, count * ROWS_ONE), :],
        )
        return block, keep

    def merge(at, weighted, top, total):
        old_top = mx[at].reshape(-1, dim)
        new_top = jnp.maximum(old_top, top)
        old_part, part = jnp.exp2(old_top - new_top), jnp.exp2(top - new_top)
        return (
            acc[at].reshape(-1, dim) * old_part + weighted * part,
            new_top,
            sm[at].reshape(-1, dim) * old_part + total * part,
        )

    def two(s, b, bias=None):
        bias = bias2 if bias is None else bias
        part = pl.ds(s * RATIO, RATIO)
        own = pl.ds(pl.multiple_of(b * ROWS_TWO, ROWS_TWO), ROWS_TWO)
        near_rows = pl.ds(pl.multiple_of(rows + (b - 1) * ROWS_TWO, ROWS_TWO), 2 * ROWS_TWO)

        def keep(found):
            merged = merge((part, own, slice(None)), *found)
            for ref, value in zip((acc, mx, sm), merged):
                ref[part, own, :] = value.reshape(RATIO, ROWS_TWO, dim)

        block = tuple(x[part, at, :].reshape(-1, dim) for x, at in ((qb, own), (kb, near_rows), (vb, near_rows)))
        return block + (bias[...],), keep

    def three(x):
        def keep(found):
            weighted, _, total = merge((x,), *found)
            ob[x] = (weighted / total).astype(ob.dtype)

        return (qb[x], kb[x], vb[x], bias3[...]), keep

    def run(*groups):
        parts = [item for items, _ in groups for item in items]
        found = iter(attend([block for block, _ in parts], scale))
        for items, after in groups:
            for _, keep in items:
                keep(next(found))
            after()

    def nothing():
        pass

    def some(items, count):
        return [items[i : i + count] for i in range(0, len(items), count)]

    steps = piece // ROWS_ONE
    soon = mine + 1 - mine % 2
    later = (group // 2, group - soon)
    near_far = 2 + jnp.where(mine == 1, 1, 0)
    edge = jnp.where(mine == last, 1, 0)
    for d in near:
        arrival(0, d).wait_recv()
    pass_on(onward_rows(0, 1))
    for d in near:
        arrival(1, d).wait_recv()
    pass_on(onward_rows(1, 1))
    for d in far:
        arrival(0, d).wait_recv()
    for d in near:
        exchange(2, d).start()
    for s in range(len(QUERY_PARTS)):
        for d in far:
            exchange(2, d, s).start()
    pass_on(onward_rows(0, 2), onward_late(0, 0), onward_early(0, 0))
    for d in far:
        arrival(1, d).wait_recv()
    pass_on(
        onward_rows(1, 2), onward_late(1, 0), onward_early(1, 0),
        *[f(x, u) for u in (1, 2) for f in (onward_late, onward_early) for x in (0, 1)],
        *[f(x, u) for f in (onward_early, onward_late) for u in (3, 4) for x in (0, 1)],
    )
    def inners(d, s=None):
        return [one(member(d) * steps + inner, 0, s) for inner in range(1, steps)]

    run((inners(0), nothing))
    for d in near:
        arrival(2, d).wait_recv()
    for d, b in zip(near, (soon, near_far)):
        run((inners(d) + [one(b * steps)], nothing))
    run(([two(s, soon) for s in range(CHUNKS)], nothing))

    @pl.when(has_prev)
    def _():
        for k in range(3):
            for which in (0, 1):
                onward_rows(which, k).wait_recv()

    def sooner(s):
        if s == CHUNKS:
            return []
        found = []
        for i, (first, _) in enumerate(QUERY_PARTS):
            for d in far if first == s else ():
                arrival(2, d, i).wait_recv()
                found += inners(d, i) + [one(member(d) * steps, jnp.where(member(d) == 0, 1, 0), i)]
        return found + [two(s, b) for b in later]


    head = tp * group + mine

    def lanes(index):
        return pl.ds(pl.multiple_of(index * dim, dim), dim)

    def give(u, d):
        part = pl.ds(*UNITS[u])
        other = member(d)
        return pltpu.make_async_remote_copy(
            src_ref=ob.at[part, span(piece * other), :],
            dst_ref=ab.at[part, :, lanes(head)],
            send_sem=o_send.at[u, d],
            recv_sem=o_recv.at[u, d],
            device_id={"sp": base + other},
            device_id_type=MESH,
        )

    def taken(u, d):
        part = pl.ds(*UNITS[u])
        return pltpu.make_async_remote_copy(
            src_ref=ob.at[part, span(0), :],
            dst_ref=ab.at[part, :, lanes(tp * group + member(d))],
            send_sem=o_send.at[u, d],
            recv_sem=o_recv.at[u, d],
            device_id={"sp": sp},
            device_id_type=MESH,
        )

    def swap(u, d):
        part = pl.ds(*UNITS[u])
        slot = ab.at[part, :, lanes(tp * group + member(d))]
        return pltpu.make_async_remote_copy(
            src_ref=ob.at[part, span(piece * mine), :] if d == 0 else slot,
            dst_ref=slot,
            send_sem=d_send.at[u, d],
            recv_sem=d_recv.at[u, d],
            device_id={"tp": partner},
            device_id_type=MESH,
        )

    def swapped(u, d):
        part = pl.ds(*UNITS[u])
        return pltpu.make_async_remote_copy(
            src_ref=ob.at[part, span(0), :],
            dst_ref=ab.at[part, :, lanes(partner * group + member(d))],
            send_sem=d_send.at[u, d],
            recv_sem=d_recv.at[u, d],
            device_id={"tp": partner},
            device_id_type=MESH,
        )

    def hand_over(u):
        for d in range(1, group):
            taken(u, d).wait_recv()
            swap(u, d).start()

    def project(u):
        start, count = UNITS[u]
        for d in range(group):
            swapped(u, d).wait_recv()
        attended = ab[pl.ds(start, count)].reshape(count * piece, -1)
        mixed = jnp.dot(attended, w_ref[...], preferred_element_type=jnp.float32)
        for c in range(mixed.shape[1] // dim):
            for j in range(count):
                residue = (start + j) // RATIO + (start + j) % RATIO * DILATION_TWO
                at = pl.ds(residue, piece, stride=res + 1)
                nat[c, at, :] = mixed[j * piece : (j + 1) * piece, c * dim : (c + 1) * dim]

    def from_prev(*copies):
        @pl.when(has_prev)
        def _():
            for copy in copies:
                copy.wait_recv()

    def hand_out(u):
        def now():
            part = pl.ds(*UNITS[u])
            for d in far + near:
                give(u, d).start()
            swap(u, 0).start()
            ab[part, :, lanes(head)] = ob[part, span(piece * mine), :]

        return now

    def threes(u):
        start, count = UNITS[u]
        return [three(x) for x in range(start, start + count)]

    for s in range(CHUNKS):
        units = [u for u, (start, _) in enumerate(UNITS) if start // RATIO == s]
        from_prev(*[onward_early(x, u) for u in units for x in (0, 1)])
        from_prev(*[onward_late(x, units[0]) for x in (0, 1)])
        edges = [one(edge * steps, 1 - edge)] if s == 0 else []
        run((edges + sooner(s), nothing), ([two(s, 0, bias2f)] + threes(units[0]), hand_out(units[0])))
        for u in units[1:]:
            from_prev(*[onward_late(x, u) for x in (0, 1)])
            run((threes(u), hand_out(u)))
        if s == 2:
            hand_over(0)
    loads[3].wait()
    for u in range(1, len(UNITS)):
        hand_over(u)
        project(u - 1)
    project(len(UNITS) - 1)

    per = piece // PARTS
    for i in range(piece):
        for c in range(nat.shape[0]):
            o_refs[i // per][i % per * res : i % per * res + res, c * dim : (c + 1) * dim] = nat[
                c, i * (res + 1) : i * (res + 1) + res, :
            ].astype(jnp.bfloat16)

    for which in (0, 1):
        for d in range(1, group):
            exchange(which, d).wait_send()
    for d in near:
        exchange(2, d).wait_send()
    for d in far:
        for s in range(len(QUERY_PARTS)):
            exchange(2, d, s).wait_send()

    @pl.when(has_next)
    def _():
        for which in (0, 1):
            for k in range(3):
                onward_rows(which, k).wait_send()
            for u in range(len(UNITS)):
                onward_early(which, u).wait_send()
                onward_late(which, u).wait_send()

    for u in range(len(UNITS)):
        for d in range(1, group):
            give(u, d).wait_send()
        for d in range(group):
            swap(u, d).wait_send()


def local(queries, keys, values, w_out):
    tokens, group, dim = queries.shape
    features, columns = w_out.shape
    res = DILATION_THREE
    piece = tokens // res
    rows = group * piece
    assert group == 4 and piece > ROWS_ONE
    assert group * tokens == WINDOW_THREE and lax.axis_size("sp") % group == 0 and lax.axis_size("tp") == 2

    low, full = jnp.bfloat16, jnp.float32
    dma = pltpu.SemaphoreType.DMA
    vmem = pl.BlockSpec(memory_space=pltpu.VMEM)
    hbm = pl.BlockSpec(memory_space=pltpu.HBM)
    mixed = pl.pallas_call(
        functools.partial(kernel, group),
        out_shape=[jax.ShapeDtypeStruct((tokens // PARTS, columns), low)] * PARTS,
        in_specs=[hbm] * 4,
        out_specs=[vmem] * PARTS,
        scratch_shapes=[
            pltpu.VMEM((columns // dim, piece * (res + 1), dim), full),
            pltpu.VMEM((3, tokens, group, dim), low),
            pltpu.VMEM((3, piece * (res + 1) * group, dim), full),
            pltpu.VMEM((group, res, piece, dim), low),
            pltpu.VMEM((group, res, piece, dim), low),
            pltpu.VMEM((group, res, piece, dim), low),
            pltpu.VMEM((features, columns), low),
            pltpu.VMEM((res, rows, dim), low),
            pltpu.VMEM((res, 2 * rows, dim), low),
            pltpu.VMEM((res, 2 * rows, dim), low),
            pltpu.VMEM((res, rows, dim), full),
            pltpu.VMEM((res, rows, dim), full),
            pltpu.VMEM((res, rows, dim), full),
            pltpu.VMEM((res, rows, dim), low),
            pltpu.VMEM((res, piece, features), low),
            pltpu.VMEM((2, res * ROWS_ONE, 2 * res * ROWS_ONE), full),
            pltpu.VMEM((RATIO * ROWS_TWO, 2 * RATIO * ROWS_TWO), full),
            pltpu.VMEM((RATIO * ROWS_TWO, 2 * RATIO * ROWS_TWO), full),
            pltpu.VMEM((rows, 2 * rows), full),
            dma((4,)),
            dma((3, group)), dma((3, group)),
            dma((len(QUERY_PARTS),)), dma((len(QUERY_PARTS),)),
            dma((2, 3)), dma((2, 3)),
            dma((2, len(UNITS))), dma((2, len(UNITS))),
            dma((2, len(UNITS))), dma((2, len(UNITS))),
            dma((len(UNITS), group)), dma((len(UNITS), group)),
            dma((len(UNITS), group)), dma((len(UNITS), group)),
        ],
        compiler_params=pltpu.CompilerParams(
            collective_id=0, has_side_effects=True, vmem_limit_bytes=55_000_000
        ),
    )(queries, keys, values, w_out)
    return jnp.concatenate(mixed, axis=0)


def solution(mesh):
    in_specs = (P("sp", "tp", None), P("sp", "tp", None), P("sp", "tp", None), P(None, "tp"))
    out_specs = P("sp", "tp")
    return jax.shard_map(local, mesh=mesh, in_specs=in_specs, out_specs=out_specs, check_vma=False)
```

```python
import functools
import math

import jax
import jax.numpy as jnp
from jax import lax
from jax.experimental import pallas as pl
from jax.experimental.pallas import tpu as pltpu
from jax.sharding import PartitionSpec as P

W1 = 128
WINDOW_TWO = 512
DILATION_TWO = 4
WINDOW_THREE = 2048
DILATION_THREE = 16
MESH = pl.DeviceIdType.MESH
RATIO = DILATION_THREE // DILATION_TWO
CHUNKS = DILATION_TWO
ROWS_ONE = 16
PARTS = 2
QUERY_PARTS = ((0, 1), (1, 3))
UNITS = ((0, 4), (4, 4), (8, 4), (12, 2), (14, 2))
ROWS_TWO = WINDOW_TWO // DILATION_THREE


def attend(blocks, scale):
    scores = [
        lax.dot_general(q, k, (((1,), (1,)), ((), ())), preferred_element_type=jnp.float32)
        for q, k, _, _ in blocks
    ]
    scores = [bias(x * scale) if callable(bias) else x * scale + bias for x, (_, _, _, bias) in zip(scores, blocks)]
    tops = [jnp.max(x, axis=-1, keepdims=True) for x in scores]
    numerators = [jnp.exp2(x - top) for x, top in zip(scores, tops)]
    sums = [jnp.sum(x, axis=-1, keepdims=True) for x in numerators]
    weighted = [
        jnp.dot(x.astype(v.dtype), v, preferred_element_type=jnp.float32)
        for x, (_, _, v, _) in zip(numerators, blocks)
    ]
    return [
        (x, jnp.broadcast_to(top, x.shape), jnp.broadcast_to(total, x.shape))
        for x, top, total in zip(weighted, tops, sums)
    ]


def bias_of(shape, place_q, place_k, first_own, window, has_prev):
    query_place, _ = place_q(lax.broadcasted_iota(jnp.int32, shape, 0))
    key_place, key_row = place_k(lax.broadcasted_iota(jnp.int32, shape, 1))
    distance = query_place - key_place
    allowed = (distance >= 0) & (distance <= window)
    general = jnp.where(allowed, 0.0, -jnp.inf).astype(jnp.float32)
    gate = jnp.where(has_prev, 0, first_own)
    first = jnp.where(allowed & (key_row >= gate), 0.0, -jnp.inf).astype(jnp.float32)
    return general, first


def kernel(
    group, q_hbm, k_hbm, v_hbm, w_hbm, *refs
):
    o_refs = refs[:PARTS]
    (
    nat, raw, wide, q_ref, k_ref, v_ref, w_ref, qb, kb, vb, acc, mx, sm, ob, ab, bias1, bias2, bias2f,
    load, in_send, in_recv, q_send, q_recv, z_send, z_recv, zb_send, zb_recv, zc_send, zc_recv, o_send, o_recv, d_send, d_recv,
    ) = refs[PARTS:]
    res, dim = DILATION_THREE, q_ref.shape[-1]
    piece = q_ref.shape[2]
    rows = group * piece
    sp, tp = lax.axis_index("sp"), lax.axis_index("tp")
    n_sp, n_tp = lax.axis_size("sp"), lax.axis_size("tp")
    mine = lax.rem(sp, group)
    base = sp - mine
    has_prev = sp >= group
    has_next = sp + group < n_sp
    partner = n_tp - 1 - tp
    scale = math.log2(math.e) / math.sqrt(dim)

    loads = [
        pltpu.make_async_copy(source, place, load.at[i])
        for i, (source, place) in enumerate(
            ((k_hbm, raw.at[0]), (v_hbm, raw.at[1]), (q_hbm, raw.at[2]), (w_hbm, w_ref))
        )
    ]
    barrier = pltpu.get_barrier_semaphore()
    for d in range(1, group):
        pl.semaphore_signal(
            barrier, inc=1, device_id={"sp": base + lax.rem(mine + d, group)}, device_id_type=MESH
        )
    pl.semaphore_signal(barrier, inc=1, device_id={"tp": partner}, device_id_type=MESH)

    @pl.when(has_prev)
    def _():
        pl.semaphore_signal(barrier, inc=1, device_id={"sp": sp - group}, device_id_type=MESH)

    @pl.when(has_next)
    def _():
        pl.semaphore_signal(barrier, inc=1, device_id={"sp": sp + group}, device_id_type=MESH)

    for copy in loads:
        copy.start()

    def span(start):
        return pl.ds(pl.multiple_of(start, piece), piece)

    tensors = ((k_ref, kb, rows), (v_ref, vb, rows), (q_ref, qb, 0))

    def member(d):
        other, bit = mine, 1
        while bit <= d:
            if d & bit:
                other = other + bit * (1 - 2 * lax.rem(mine // bit, 2))
            bit *= 2
        return other

    def exchange(which, d, s=None):
        source, buffer, offset = tensors[which]
        other = member(d)
        part = slice(None) if s is None else pl.ds(*(x * RATIO for x in QUERY_PARTS[s]))
        return pltpu.make_async_remote_copy(
            src_ref=source.at[other, part],
            dst_ref=buffer.at[part, span(offset + piece * mine), :],
            send_sem=in_send.at[which, d] if s is None else q_send.at[s],
            recv_sem=in_recv.at[which, d] if s is None else q_recv.at[s],
            device_id={"sp": base + other},
            device_id_type=MESH,
        )

    def arrival(which, d, s=None):
        source, buffer, offset = tensors[which]
        part = slice(None) if s is None else pl.ds(*(x * RATIO for x in QUERY_PARTS[s]))
        return pltpu.make_async_remote_copy(
            src_ref=source.at[0, part],
            dst_ref=buffer.at[part, span(offset + piece * member(d)), :],
            send_sem=in_send.at[which, d] if s is None else q_send.at[s],
            recv_sem=in_recv.at[which, d] if s is None else q_recv.at[s],
            device_id={"sp": sp},
            device_id_type=MESH,
        )

    low = piece - ROWS_ONE

    last = group - 1
    swapped_roles = member(2) == last
    early = jnp.where(swapped_roles, member(2), member(3))
    late = jnp.where(swapped_roles, member(3), member(2))

    def onward(which, src, dst, send, recv):
        return pltpu.make_async_remote_copy(
            src_ref=src,
            dst_ref=dst,
            send_sem=send,
            recv_sem=recv,
            device_id={"sp": sp + group},
            device_id_type=MESH,
        )

    def onward_rows(which, k):
        source, buffer, _ = tensors[which]
        start = piece * (mine, member(1), early)[k]
        if k == 0:
            src, dst = source.at[mine], buffer.at[:, span(start), :]
        elif k == 1:
            src, dst = buffer.at[:, span(rows + start), :], buffer.at[:, span(start), :]
        else:
            ends = [pl.ds(pl.multiple_of(x + start + low, ROWS_ONE), ROWS_ONE) for x in (rows, 0)]
            src, dst = (buffer.at[:, x, :] for x in ends)
        return onward(which, src, dst, z_send.at[which, k], z_recv.at[which, k])

    def onward_early(which, u):
        _, buffer, _ = tensors[which]
        ends = [pl.ds(pl.multiple_of(x + piece * early, ROWS_ONE), low) for x in (rows, 0)]
        src, dst = (buffer.at[pl.ds(*UNITS[u]), x, :] for x in ends)
        return onward(which, src, dst, zc_send.at[which, u], zc_recv.at[which, u])

    def onward_late(which, u):
        _, buffer, _ = tensors[which]
        src, dst = (buffer.at[pl.ds(*UNITS[u]), span(x + piece * late), :] for x in (rows, 0))
        return onward(which, src, dst, zb_send.at[which, u], zb_recv.at[which, u])

    near = [d for d in range(1, group) if d & (d - 1) == 0]
    far = [d for d in range(1, group) if d & (d - 1)]
    pad = (res + 1) * group
    for which, (source, buffer, offset) in enumerate(tensors):
        loads[which].wait()
        for i in range(piece):
            tokens = raw[which, pl.ds(i * res, res)].astype(jnp.float32)
            wide[which, pl.ds(i * pad, res * group), :] = tokens.reshape(res * group, dim)
        for h in range(group):
            for r in range(res):
                store = r % DILATION_TWO * RATIO + r // DILATION_TWO
                rows_of = wide[which, pl.ds(r * group + h, piece, stride=pad), :]
                source[h, store] = rows_of.astype(source.dtype)
        buffer[:, span(offset + piece * mine), :] = source[mine]

    @pl.when(jnp.logical_not(has_prev))
    def _():
        kb[:, :rows, :] = jnp.zeros((res, rows, dim), kb.dtype)
        vb[:, :rows, :] = jnp.zeros((res, rows, dim), vb.dtype)

    def place_one(per):
        def place(i):
            store, row = i // per, i % per
            residue = (store % RATIO) * DILATION_TWO + store // RATIO
            return row * res + residue, row
        return place

    def place_two(per):
        def place(i):
            j, row = i // per, i % per
            return row * RATIO + j, row
        return place

    def shifted(place, by):
        def moved(i):
            at, row = place(i)
            return at + by, row
        return moved

    bias1[0], bias1[1] = bias_of(
        bias1.shape[1:], shifted(place_one(ROWS_ONE), ROWS_ONE * res), place_one(2 * ROWS_ONE), ROWS_ONE, W1, has_prev
    )
    bias2[...], bias2f[...] = bias_of(
        bias2.shape, shifted(place_two(ROWS_TWO), ROWS_TWO * RATIO), place_two(2 * ROWS_TWO), ROWS_TWO,
        WINDOW_TWO // DILATION_TWO, has_prev,
    )
    pl.semaphore_wait(barrier, group + jnp.where(has_prev, 1, 0) + jnp.where(has_next, 1, 0))

    @pl.when(has_next)
    def _():
        for which in (0, 1):
            onward_rows(which, 0).start()

    for members in (near, far):
        for which in (0, 1):
            for d in members:
                exchange(which, d).start()

    def pass_on(*copies):
        @pl.when(has_next)
        def _():
            for copy in copies:
                copy.start()

    def one(b, first=0, s=None):
        own = pl.ds(pl.multiple_of(b * ROWS_ONE, ROWS_ONE), ROWS_ONE)
        near_rows = pl.ds(pl.multiple_of(rows + (b - 1) * ROWS_ONE, ROWS_ONE), 2 * ROWS_ONE)
        start, count = (0, res) if s is None else (x * RATIO for x in QUERY_PARTS[s])
        part = pl.ds(start, count)

        def keep(found):
            for ref, value in zip((acc, mx, sm), found):
                ref[part, own, :] = value.reshape(count, ROWS_ONE, dim)

        block = (
            qb[part, own, :].reshape(-1, dim),
            kb[:, near_rows, :].reshape(-1, dim),
            vb[:, near_rows, :].reshape(-1, dim),
            bias1[first, pl.ds(start * ROWS_ONE, count * ROWS_ONE), :],
        )
        return block, keep

    def merge(at, weighted, top, total):
        old_top = mx[at].reshape(-1, dim)
        new_top = jnp.maximum(old_top, top)
        old_part, part = jnp.exp2(old_top - new_top), jnp.exp2(top - new_top)
        return (
            acc[at].reshape(-1, dim) * old_part + weighted * part,
            new_top,
            sm[at].reshape(-1, dim) * old_part + total * part,
        )

    def two(s, b, bias=None):
        bias = bias2 if bias is None else bias
        part = pl.ds(s * RATIO, RATIO)
        own = pl.ds(pl.multiple_of(b * ROWS_TWO, ROWS_TWO), ROWS_TWO)
        near_rows = pl.ds(pl.multiple_of(rows + (b - 1) * ROWS_TWO, ROWS_TWO), 2 * ROWS_TWO)

        def keep(found):
            merged = merge((part, own, slice(None)), *found)
            for ref, value in zip((acc, mx, sm), merged):
                ref[part, own, :] = value.reshape(RATIO, ROWS_TWO, dim)

        block = tuple(x[part, at, :].reshape(-1, dim) for x, at in ((qb, own), (kb, near_rows), (vb, near_rows)))
        return block + (bias[...],), keep

    ahead = [lax.broadcasted_iota(jnp.int32, (rows, rows), i) for i in (1, 0)]
    ahead = ahead[0] - ahead[1]
    gate = jnp.where(has_prev, 0, rows)

    def band(x):
        earlier = jnp.where(ahead >= gate, x[:, :rows], -jnp.inf)
        return jnp.concatenate([earlier, jnp.where(ahead <= 0, x[:, rows:], -jnp.inf)], axis=1)

    def three(x):
        def keep(found):
            weighted, _, total = merge((x,), *found)
            ob[x] = (weighted / total).astype(ob.dtype)

        return (qb[x], kb[x], vb[x], band), keep

    def run(*groups):
        parts = [item for items, _ in groups for item in items]
        found = iter(attend([block for block, _ in parts], scale))
        for items, after in groups:
            for _, keep in items:
                keep(next(found))
            after()

    def nothing():
        pass

    def some(items, count):
        return [items[i : i + count] for i in range(0, len(items), count)]

    steps = piece // ROWS_ONE
    soon = mine + 1 - mine % 2
    later = (group // 2, group - soon)
    near_far = 2 + jnp.where(mine == 1, 1, 0)
    edge = jnp.where(mine == last, 1, 0)
    for d in near:
        arrival(0, d).wait_recv()
    pass_on(onward_rows(0, 1))
    for d in near:
        arrival(1, d).wait_recv()
    pass_on(onward_rows(1, 1))
    for d in far:
        arrival(0, d).wait_recv()
    for d in near:
        exchange(2, d).start()
    for s in range(len(QUERY_PARTS)):
        for d in far:
            exchange(2, d, s).start()
    pass_on(onward_rows(0, 2), onward_late(0, 0), onward_early(0, 0))
    for d in far:
        arrival(1, d).wait_recv()
    pass_on(
        onward_rows(1, 2), onward_late(1, 0), onward_early(1, 0),
        *[f(x, u) for u in (1, 2) for f in (onward_late, onward_early) for x in (0, 1)],
        *[f(x, u) for f in (onward_early, onward_late) for u in (3, 4) for x in (0, 1)],
    )
    def inners(d, s=None):
        return [one(member(d) * steps + inner, 0, s) for inner in range(1, steps)]

    run((inners(0), nothing))
    for d in near:
        arrival(2, d).wait_recv()
    for d, b in zip(near, (soon, near_far)):
        run((inners(d) + [one(b * steps)], nothing))

    @pl.when(has_prev)
    def _():
        for k in range(3):
            for which in (0, 1):
                onward_rows(which, k).wait_recv()

    def sooner(s):
        if s == CHUNKS:
            return []
        found = []
        for i, (first, _) in enumerate(QUERY_PARTS):
            for d in far if first == s else ():
                arrival(2, d, i).wait_recv()
                found += inners(d, i) + [one(member(d) * steps, jnp.where(member(d) == 0, 1, 0), i)]
        return found + [two(s, b) for b in (soon, *later)]


    head = tp * group + mine

    def lanes(index):
        return pl.ds(pl.multiple_of(index * dim, dim), dim)

    def give(u, d):
        part = pl.ds(*UNITS[u])
        other = member(d)
        return pltpu.make_async_remote_copy(
            src_ref=ob.at[part, span(piece * other), :],
            dst_ref=ab.at[part, :, lanes(head)],
            send_sem=o_send.at[u, d],
            recv_sem=o_recv.at[u, d],
            device_id={"sp": base + other},
            device_id_type=MESH,
        )

    def taken(u, d):
        part = pl.ds(*UNITS[u])
        return pltpu.make_async_remote_copy(
            src_ref=ob.at[part, span(0), :],
            dst_ref=ab.at[part, :, lanes(tp * group + member(d))],
            send_sem=o_send.at[u, d],
            recv_sem=o_recv.at[u, d],
            device_id={"sp": sp},
            device_id_type=MESH,
        )

    def swap(u, d):
        part = pl.ds(*UNITS[u])
        slot = ab.at[part, :, lanes(tp * group + member(d))]
        return pltpu.make_async_remote_copy(
            src_ref=ob.at[part, span(piece * mine), :] if d == 0 else slot,
            dst_ref=slot,
            send_sem=d_send.at[u, d],
            recv_sem=d_recv.at[u, d],
            device_id={"tp": partner},
            device_id_type=MESH,
        )

    def swapped(u, d):
        part = pl.ds(*UNITS[u])
        return pltpu.make_async_remote_copy(
            src_ref=ob.at[part, span(0), :],
            dst_ref=ab.at[part, :, lanes(partner * group + member(d))],
            send_sem=d_send.at[u, d],
            recv_sem=d_recv.at[u, d],
            device_id={"tp": partner},
            device_id_type=MESH,
        )

    def hand_over(u):
        for d in range(1, group):
            taken(u, d).wait_recv()
            swap(u, d).start()

    def project(u):
        start, count = UNITS[u]
        for d in range(group):
            swapped(u, d).wait_recv()
        attended = ab[pl.ds(start, count)].reshape(count * piece, -1)
        mixed = jnp.dot(attended, w_ref[...], preferred_element_type=jnp.float32)
        for c in range(mixed.shape[1] // dim):
            for j in range(count):
                residue = (start + j) // RATIO + (start + j) % RATIO * DILATION_TWO
                at = pl.ds(residue, piece, stride=res + 1)
                nat[c, at, :] = mixed[j * piece : (j + 1) * piece, c * dim : (c + 1) * dim]

    def from_prev(*copies):
        @pl.when(has_prev)
        def _():
            for copy in copies:
                copy.wait_recv()

    def hand_out(u):
        def now():
            part = pl.ds(*UNITS[u])
            for d in far + near:
                give(u, d).start()
            swap(u, 0).start()
            ab[part, :, lanes(head)] = ob[part, span(piece * mine), :]

        return now

    def threes(u):
        start, count = UNITS[u]
        return [three(x) for x in range(start, start + count)]

    for s in range(CHUNKS):
        units = [u for u, (start, _) in enumerate(UNITS) if start // RATIO == s]
        from_prev(*[onward_early(x, u) for u in units for x in (0, 1)])
        from_prev(*[onward_late(x, units[0]) for x in (0, 1)])
        edges = [one(edge * steps, 1 - edge)] if s == 0 else []
        run((edges + sooner(s), nothing), ([two(s, 0, bias2f)] + threes(units[0]), hand_out(units[0])))
        for u in units[1:]:
            from_prev(*[onward_late(x, u) for x in (0, 1)])
            run((threes(u), hand_out(u)))
    loads[3].wait()
    for u in range(len(UNITS)):
        hand_over(u)
        if u:
            project(u - 1)
    project(len(UNITS) - 1)

    per = piece // PARTS
    for i in range(piece):
        for c in range(nat.shape[0]):
            o_refs[i // per][i % per * res : i % per * res + res, c * dim : (c + 1) * dim] = nat[
                c, i * (res + 1) : i * (res + 1) + res, :
            ].astype(jnp.bfloat16)

    for which in (0, 1):
        for d in range(1, group):
            exchange(which, d).wait_send()
    for d in near:
        exchange(2, d).wait_send()
    for d in far:
        for s in range(len(QUERY_PARTS)):
            exchange(2, d, s).wait_send()

    @pl.when(has_next)
    def _():
        for which in (0, 1):
            for k in range(3):
                onward_rows(which, k).wait_send()
            for u in range(len(UNITS)):
                onward_early(which, u).wait_send()
                onward_late(which, u).wait_send()

    for u in range(len(UNITS)):
        for d in range(1, group):
            give(u, d).wait_send()
        for d in range(group):
            swap(u, d).wait_send()


def local(queries, keys, values, w_out):
    tokens, group, dim = queries.shape
    features, columns = w_out.shape
    res = DILATION_THREE
    piece = tokens // res
    rows = group * piece
    assert group == 4 and piece > ROWS_ONE
    assert group * tokens == WINDOW_THREE and WINDOW_THREE // DILATION_THREE == rows and lax.axis_size("sp") % group == 0 and lax.axis_size("tp") == 2

    low, full = jnp.bfloat16, jnp.float32
    dma = pltpu.SemaphoreType.DMA
    vmem = pl.BlockSpec(memory_space=pltpu.VMEM)
    hbm = pl.BlockSpec(memory_space=pltpu.HBM)
    mixed = pl.pallas_call(
        functools.partial(kernel, group),
        out_shape=[jax.ShapeDtypeStruct((tokens // PARTS, columns), low)] * PARTS,
        in_specs=[hbm] * 4,
        out_specs=[vmem] * PARTS,
        scratch_shapes=[
            pltpu.VMEM((columns // dim, piece * (res + 1), dim), full),
            pltpu.VMEM((3, tokens, group, dim), low),
            pltpu.VMEM((3, piece * (res + 1) * group, dim), full),
            pltpu.VMEM((group, res, piece, dim), low),
            pltpu.VMEM((group, res, piece, dim), low),
            pltpu.VMEM((group, res, piece, dim), low),
            pltpu.VMEM((features, columns), low),
            pltpu.VMEM((res, rows, dim), low),
            pltpu.VMEM((res, 2 * rows, dim), low),
            pltpu.VMEM((res, 2 * rows, dim), low),
            pltpu.VMEM((res, rows, dim), full),
            pltpu.VMEM((res, rows, dim), full),
            pltpu.VMEM((res, rows, dim), full),
            pltpu.VMEM((res, rows, dim), low),
            pltpu.VMEM((res, piece, features), low),
            pltpu.VMEM((2, res * ROWS_ONE, 2 * res * ROWS_ONE), full),
            pltpu.VMEM((RATIO * ROWS_TWO, 2 * RATIO * ROWS_TWO), full),
            pltpu.VMEM((RATIO * ROWS_TWO, 2 * RATIO * ROWS_TWO), full),
            dma((4,)),
            dma((3, group)), dma((3, group)),
            dma((len(QUERY_PARTS),)), dma((len(QUERY_PARTS),)),
            dma((2, 3)), dma((2, 3)),
            dma((2, len(UNITS))), dma((2, len(UNITS))),
            dma((2, len(UNITS))), dma((2, len(UNITS))),
            dma((len(UNITS), group)), dma((len(UNITS), group)),
            dma((len(UNITS), group)), dma((len(UNITS), group)),
        ],
        compiler_params=pltpu.CompilerParams(
            collective_id=0, has_side_effects=True, vmem_limit_bytes=55_000_000
        ),
    )(queries, keys, values, w_out)
    return jnp.concatenate(mixed, axis=0)


def solution(mesh):
    in_specs = (P("sp", "tp", None), P("sp", "tp", None), P("sp", "tp", None), P(None, "tp"))
    out_specs = P("sp", "tp")
    return jax.shard_map(local, mesh=mesh, in_specs=in_specs, out_specs=out_specs, check_vma=False)
```
